32 devices in a mesh: sp: 8 (over z, y), tp: 4 (over x, core).
Axes of the slice: x: 2, y: 2, z: 4, core: 2. Of those that a mesh axis runs over, the one named last changes fastest.
Arguments:
- glu_value: bfloat16 [8192, 1024], P('sp', 'tp'), may hold values from -6 to 6
- glu_gate: bfloat16 [8192, 1024], P('sp', 'tp'), may hold values from -8 to 8
- conv_taps: float32 [31, 1024], P(None, 'tp'), may hold values from -1 to 1
- channel_gain: float32 [1024], P('tp'), may hold values from 0.1 to 1.9
- proj_weight: bfloat16 [1024, 1024], P('tp'), may hold values from -0.1875 to 0.1875
- out_grad: bfloat16 [8192, 1024], P('sp'), may hold values from -6 to 6
Outputs:
- value_grad: bfloat16 [8192, 1024], P('sp', 'tp')
- gate_grad: bfloat16 [8192, 1024], P('sp', 'tp')
- proj_grad: float32 [1024, 1024], P(('tp', 'sp'))
- taps_grad: float32 [31, 1024], P(None, 'tp')
- norm_gain_gradient: float32 [1024], P('tp')
The draws below stay inside these ranges and needn't reach their ends.
All inputs are finite; a program needn't handle non-finite values.
Results may differ from the reference program's by a relative error of at most 0.0029.
Values may be sent and summed in bfloat16 or wider, within the bound.
A program may use at most 64 MiB of HBM per device.

```python
import jax
import jax.numpy as jnp
from jax import lax

CH = 1024
KERNEL = 31
TOKENS = 8192


def levels(key, shape, split, low, high):
    def one(position, blocks):
        draws = jax.random.uniform(jax.random.fold_in(jax.random.fold_in(key, 6), position), (blocks,), jnp.float32, low / len(split), high / len(split))
        return jnp.repeat(jnp.exp(draws), shape[position] // blocks).reshape((-1,) + (1,) * (len(shape) - position - 1))

    loudness = one(*split[0])
    for cut in split[1:]:
        loudness = loudness * one(*cut)
    return loudness


def centred(stream_key, shape, spread, most, split=(), dtype=jnp.bfloat16):
    entries = spread * jax.random.normal(stream_key, shape, jnp.float32)
    if split:
        entries = entries * levels(stream_key, shape, split, -0.22, 0.18)
    return jnp.clip(entries, -most, most).astype(dtype)


def setup_inputs(seed: int = 0) -> dict:
    key_of = jax.random.split(jax.random.key(seed), 7)
    return {
        "glu_value": centred(key_of[0], (TOKENS, CH), 1.0, 6.0, ((0, 8), (1, 4))),
        "glu_gate": centred(key_of[1], (TOKENS, CH), 1.5, 8.0, ((0, 8), (1, 4))),
        "conv_taps": centred(key_of[2], (KERNEL, CH), KERNEL ** -0.5, 1.0, ((1, 4),), jnp.float32),
        "channel_gain": jnp.clip(1.0 + 0.18 * jax.random.normal(key_of[3], (CH,), jnp.float32), 0.1, 1.9),
        "proj_weight": centred(key_of[4], (CH, CH), CH ** -0.5, 0.1875, ((0, 4),)),
        "out_grad": centred(key_of[5], (TOKENS, CH), 1.0, 6.0, ((0, 8),)),
    }


def reference(glu_value, glu_gate, conv_taps, channel_gain, proj_weight, out_grad):
    halo_rows = KERNEL - 1
    row_count = glu_value.shape[0]
    value_f = glu_value.astype(jnp.float32)
    gate_sig = jax.nn.sigmoid(glu_gate.astype(jnp.float32))
    glu_out = value_f * gate_sig
    padded = jnp.pad(glu_out, ((halo_rows, 0), (0, 0)))
    convolved_output = jnp.zeros_like(glu_out)
    for tap in range(KERNEL):
        convolved_output = convolved_output + conv_taps[tap] * padded[tap:tap + row_count]
    row_average = lax.optimization_barrier(jnp.mean(convolved_output, axis=1, keepdims=True))
    row_sq = lax.optimization_barrier(jnp.mean(convolved_output * convolved_output, axis=1, keepdims=True))
    inverse_deviation = lax.rsqrt(row_sq - row_average * row_average + 1e-05)
    centered_scaled = (convolved_output - row_average) * inverse_deviation
    normalized_rows = centered_scaled * channel_gain
    activ = jax.nn.silu(normalized_rows).astype(jnp.bfloat16)
    act_grad = jnp.dot(out_grad, proj_weight.T, preferred_element_type=jnp.float32)
    norm_sig = jax.nn.sigmoid(normalized_rows)
    normalized_gradient = act_grad * norm_sig * (1.0 + normalized_rows * (1.0 - norm_sig))
    centered_scaled_gradient = normalized_gradient * channel_gain
    convolved_gradient = inverse_deviation * (centered_scaled_gradient - lax.optimization_barrier(jnp.mean(centered_scaled_gradient, axis=1, keepdims=True)) - centered_scaled * lax.optimization_barrier(jnp.mean(centered_scaled_gradient * centered_scaled, axis=1, keepdims=True)))
    gradient_factor = 1.0 / jnp.sqrt(jnp.float32(row_count))
    norm_gain_gradient = lax.optimization_barrier(jnp.sum(normalized_gradient * centered_scaled, axis=0)) * gradient_factor
    taps_grad = jnp.stack([lax.optimization_barrier(jnp.sum(convolved_gradient * padded[tap:tap + row_count], axis=0)) for tap in range(KERNEL)]) * gradient_factor
    grad_pad = jnp.pad(convolved_gradient, ((0, halo_rows), (0, 0)))
    glu_grad = jnp.zeros_like(glu_out)
    for tap in range(KERNEL):
        glu_grad = glu_grad + conv_taps[tap] * grad_pad[halo_rows - tap:halo_rows - tap + row_count]
    value_grad = (glu_grad * gate_sig).astype(jnp.bfloat16)
    gate_grad = (glu_grad * value_f * gate_sig * (1.0 - gate_sig)).astype(jnp.bfloat16)
    proj_grad = jnp.dot(activ.T, out_grad, preferred_element_type=jnp.float32) * gradient_factor
    return (value_grad, gate_grad, proj_grad, taps_grad, norm_gain_gradient)
```

```python
import functools

import jax
import jax.numpy as jnp
from jax import lax
from jax.experimental import pallas as pl
from jax.experimental.pallas import tpu as pltpu

MESH = pl.DeviceIdType.MESH
F32 = jnp.float32
BF16 = jnp.bfloat16
LANES = 128
BLOCK = 128


def split_two(x):
    hi = x.astype(BF16)
    return hi, (x - hi.astype(F32)).astype(BF16)


def split_three(x):
    hi = x.astype(BF16).astype(F32)
    rest = x - hi
    mid = rest.astype(BF16).astype(F32)
    low = (rest - mid).astype(BF16).astype(F32)
    return [hi, mid, low]


def nt(a, b):
    return lax.dot_general(a, b, (((1,), (1,)), ((), ())), preferred_element_type=F32)


def nn(a, b):
    return lax.dot_general(a, b, (((1,), (0,)), ((), ())), preferred_element_type=F32)


def kernel(
    cfg,
    value_hbm, gate_hbm, taps_ref, gain_ref, weight_hbm, cot_hbm,
    vgrad_hbm, ggrad_hbm, proj_out, taps_out,
    value_v, gate_v, weight_v, cot_v, halo_v, halo_g, gsig, glu, xbuf, cg, act_t,
    taps_b, taps_acc, st1, st1_in, st2, st2_in, rs_send, rs_own, rs_in,
    tg_send, tg_in, vout, gout,
    in_sem, out_sem, halo_send, halo_recv, cgs_send, cgs_recv,
    s1_send, s1_recv, s2_send, s2_recv, rs_ssem, rs_rsem, tg_ssem, tg_rsem,
):
    rows, width, klen, halo, n_sp, n_tp, fused = cfg
    halves = width // LANES
    blocks = rows // BLOCK
    channels = width * n_tp
    lead = halo - (klen - 1)
    factor = 1.0 / jnp.sqrt(F32(rows * n_sp))
    sp = lax.axis_index("sp")
    tp = lax.axis_index("tp")

    loads = [
        pltpu.make_async_copy(src, dst, in_sem.at[i])
        for i, (src, dst) in enumerate(
            [(value_hbm, value_v), (gate_hbm, gate_v), (weight_hbm, weight_v), (cot_hbm, cot_v)]
        )
    ]
    for copy in loads:
        copy.start()

    barrier = pltpu.get_barrier_semaphore()
    sp_hops = list(range(1, n_sp)) if fused else [1, n_sp - 1]
    for o in sp_hops:
        pl.semaphore_signal(
            barrier, inc=1, device_id=(lax.rem(sp + o, n_sp), tp), device_id_type=MESH
        )
    for o in range(1, n_tp):
        pl.semaphore_signal(
            barrier, inc=1, device_id=(sp, lax.rem(tp + o, n_tp)), device_id_type=MESH
        )

    for k in range(klen):
        taps_b[k] = jnp.broadcast_to(taps_ref[k : k + 1, :], (8, width))
    taps_acc[...] = jnp.zeros_like(taps_acc)
    st1[...] = jnp.zeros_like(st1)
    st2[...] = jnp.zeros_like(st2)

    loads[0].wait()
    loads[1].wait()
    pl.semaphore_wait(barrier, len(sp_hops) + n_tp - 1)

    nxt = (jnp.minimum(sp + 1, n_sp - 1), tp)
    prv = (jnp.maximum(sp - 1, 0), tp)

    def halo_copies():
        tail = pl.ds(rows - halo, halo)
        return [
            pltpu.make_async_remote_copy(
                src_ref=src.at[tail], dst_ref=dst, send_sem=halo_send.at[i],
                recv_sem=halo_recv.at[i], device_id=nxt, device_id_type=MESH,
            )
            for i, (src, dst) in enumerate([(value_v, halo_v), (gate_v, halo_g)])
        ]

    @pl.when(sp < n_sp - 1)
    def _():
        for copy in halo_copies():
            copy.start()

    def rows_of(c):
        return pl.ds(pl.multiple_of(c * BLOCK, BLOCK), BLOCK)

    def glu_block(c, carry):
        at = rows_of(c)
        to = pl.ds(pl.multiple_of(c * BLOCK + halo, 8), BLOCK)
        sig = jax.nn.sigmoid(gate_v[at, :].astype(F32))
        out = value_v[at, :].astype(F32) * sig
        for h in range(halves):
            cols = slice(h * LANES, (h + 1) * LANES)
            gsig[h, at, :] = sig[:, cols]
            glu[h, to, :] = out[:, cols]
        return carry

    lax.fori_loop(0, blocks, glu_block, 0)

    def conv_block(src, h, base, first, tap_of):
        cols = slice(h * LANES, (h + 1) * LANES)
        acc = None
        for s in range(8):
            qs = [q for q in range((first + klen + 7) // 8 + 1) if first <= 8 * q + s < first + klen]
            if not qs:
                continue
            lo = qs[0]
            span = BLOCK + 8 * (qs[-1] - lo)
            slab = src[h, pl.ds(base + (8 * lo + s), span), :]
            for q in qs:
                tap = taps_b[tap_of(8 * q + s - first), :, cols]
                part = slab[8 * (q - lo) : 8 * (q - lo) + BLOCK]
                term = part.reshape(BLOCK // 8, 8, LANES) * tap[None]
                acc = term if acc is None else acc + term
        return acc.reshape(BLOCK, LANES)

    def place_sums(ref, c, first, second):
        which = lax.broadcasted_iota(jnp.int32, (16, width), 0)
        one = jnp.where(which == c, 1.0, 0.0).astype(BF16)
        two = jnp.where(which == c + 8, 1.0, 0.0).astype(BF16)
        total = ref[...]
        for sel, x in ((one, first), (two, second)):
            hi, low = split_two(x)
            total = total + nt(sel, hi) + nt(sel, low)
        ref[...] = total

    def forward_block(c):
        base = c * BLOCK
        at = rows_of(c)
        parts = []
        for h in range(halves):
            out = conv_block(glu, h, base, lead, lambda k: k)
            xbuf[h, at, :] = out
            parts.append(out)
        x = jnp.concatenate(parts, axis=1)
        place_sums(st1, c, x, x * x)

    def fwd_loop(c, carry):
        forward_block(c)
        return carry

    lax.fori_loop(1, blocks, fwd_loop, 0)

    @pl.when(sp > 0)
    def _():
        for copy in halo_copies():
            copy.wait_recv()
        out = halo_v[...].astype(F32) * jax.nn.sigmoid(halo_g[...].astype(F32))
        for h in range(halves):
            glu[h, 0:halo, :] = out[:, h * LANES : (h + 1) * LANES]

    @pl.when(sp == 0)
    def _():
        for h in range(halves):
            glu[h, 0:halo, :] = jnp.zeros((halo, LANES), F32)

    lax.fori_loop(0, 1, fwd_loop, 0)

    def tp_copies(src, dst, ssem, rsem):
        return [
            pltpu.make_async_remote_copy(
                src_ref=src, dst_ref=dst.at[o - 1], send_sem=ssem.at[o - 1],
                recv_sem=rsem.at[o - 1], device_id=(sp, lax.rem(tp + o, n_tp)),
                device_id_type=MESH,
            )
            for o in range(1, n_tp)
        ]

    ex1 = tp_copies(st1, st1_in, s1_send, s1_recv)
    for copy in ex1:
        copy.start()
    loads[2].wait()
    loads[3].wait()

    def act_grad_block(c, carry):
        at = rows_of(c)
        out = nt(cot_v[at, :], weight_v[...])
        for h in range(halves):
            cg[h, at, :] = out[:, h * LANES : (h + 1) * LANES]
        return carry

    lax.fori_loop(0, blocks, act_grad_block, 0)
    for copy in ex1:
        copy.wait_recv()

    total = st1[...]
    for o in range(n_tp - 1):
        total = total + st1_in[o]
    mean = total[0:8] / channels
    rstd = lax.rsqrt(total[8:16] / channels - mean * mean + 1e-05)

    def columns(a, b):
        stack = split_three(a) + split_three(b)
        stack.append(jnp.zeros((LANES - 48, LANES), F32))
        return jnp.transpose(jnp.concatenate(stack, axis=0)).astype(BF16)

    def spread(cols, c):
        k = lax.broadcasted_iota(jnp.int32, (LANES, 2 * LANES), 0)
        j = lax.broadcasted_iota(jnp.int32, (LANES, 2 * LANES), 1)
        low = jnp.where(j < LANES, 0, 24)
        hit = (k == c + low) | (k == c + low + 8) | (k == c + low + 16)
        out = nn(cols, jnp.where(hit, 1.0, 0.0).astype(BF16))
        return out[:, :LANES], out[:, LANES:]

    cols1 = columns(mean, rstd)

    def norm_block(c, carry):
        at = rows_of(c)
        mean_b, rstd_b = spread(cols1, c)
        firsts, seconds, activs = [], [], []
        for h in range(halves):
            cols = slice(h * LANES, (h + 1) * LANES)
            gain = gain_ref[0:1, cols]
            xhat = (xbuf[h, at, :] - mean_b) * rstd_b
            normed = xhat * gain
            sig = jax.nn.sigmoid(normed)
            activs.append(normed * sig)
            ngrad = cg[h, at, :] * sig * (1.0 + normed * (1.0 - sig))
            xgrad = ngrad * gain
            taps_acc[klen, :, cols] += jnp.sum(
                (ngrad * xhat).reshape(BLOCK // 8, 8, LANES), axis=0
            )
            xbuf[h, at, :] = xhat
            cg[h, at, :] = xgrad
            firsts.append(xgrad)
            seconds.append(xgrad * xhat)
        place_sums(st2, c, jnp.concatenate(firsts, axis=1), jnp.concatenate(seconds, axis=1))
        activ = jnp.concatenate(activs, axis=1)
        act_t[:, at] = jnp.transpose(activ).astype(BF16)
        return carry

    lax.fori_loop(0, blocks, norm_block, 0)

    ex2 = tp_copies(st2, st2_in, s2_send, s2_recv)
    for copy in ex2:
        copy.start()

    out_cols = proj_out.shape[-1]
    tile = 256
    hops = list(range(1, n_sp)) if fused else []
    hops.sort(key=lambda o: -min(o, n_sp - o))

    def rs_copy(o, cols):
        dest = lax.rem(sp + o, n_sp)
        return pltpu.make_async_remote_copy(
            src_ref=rs_send.at[dest, :, cols], dst_ref=rs_in.at[o - 1, :, cols],
            send_sem=rs_ssem.at[o - 1], recv_sem=rs_rsem.at[o - 1],
            device_id=(dest, tp), device_id_type=MESH,
        )

    for nb in range(out_cols // tile):
        cols = slice(nb * tile, (nb + 1) * tile)
        part = nn(act_t[...], cot_v[:, cols]) * factor
        if fused:
            own = width // n_sp
            rs_own[:, :, cols] = part.reshape(n_sp, own, tile)
            rs_send[:, :, cols] = part.astype(BF16).reshape(n_sp, own, tile)
            for o in hops:
                rs_copy(o, pl.ds(nb * tile, tile)).start()
        else:
            proj_out[:, cols] = part

    for copy in ex2:
        copy.wait_recv()
    total = st2[...]
    for o in range(n_tp - 1):
        total = total + st2_in[o]
    cols2 = columns(total[0:8] / channels, total[8:16] / channels)

    def cgrad_block(c):
        at = rows_of(c)
        base = c * BLOCK
        _, rstd_b = spread(cols1, c)
        one_b, two_b = spread(cols2, c)
        for h in range(halves):
            cols = slice(h * LANES, (h + 1) * LANES)
            grad = rstd_b * (cg[h, at, :] - one_b - xbuf[h, at, :] * two_b)
            cg[h, at, :] = grad
            grad3 = grad.reshape(BLOCK // 8, 8, LANES)
            for s in range(8):
                qs = [q for q in range((lead + klen + 7) // 8 + 1) if lead <= 8 * q + s < lead + klen]
                if not qs:
                    continue
                lo = qs[0]
                span = BLOCK + 8 * (qs[-1] - lo)
                slab = glu[h, pl.ds(base + (8 * lo + s), span), :]
                for q in qs:
                    part = slab[8 * (q - lo) : 8 * (q - lo) + BLOCK]
                    prod = grad3 * part.reshape(BLOCK // 8, 8, LANES)
                    taps_acc[8 * q + s - lead, :, cols] += jnp.sum(prod, axis=0)

    def cgrad_loop(c, carry):
        cgrad_block(c)
        return carry

    lax.fori_loop(0, 1, cgrad_loop, 0)

    cg_copy = pltpu.make_async_remote_copy(
        src_ref=cg.at[:, pl.ds(0, halo), :], dst_ref=cg.at[:, pl.ds(rows, halo), :],
        send_sem=cgs_send, recv_sem=cgs_recv, device_id=prv, device_id_type=MESH,
    )

    @pl.when(sp > 0)
    def _():
        cg_copy.start()

    lax.fori_loop(1, blocks, cgrad_loop, 0)

    taps_sum = jnp.sum(taps_acc[...], axis=1) * factor
    taps_out[...] = taps_sum

    def tg_copy(o):
        return pltpu.make_async_remote_copy(
            src_ref=tg_send, dst_ref=tg_in.at[o - 1],
            send_sem=tg_ssem.at[o - 1], recv_sem=tg_rsem.at[o - 1],
            device_id=(lax.rem(sp + o, n_sp), tp), device_id_type=MESH,
        )

    if fused:
        tg_send[...] = taps_sum.astype(BF16)
        for o in hops:
            tg_copy(o).start()

    def out_copies(c):
        at = rows_of(c)
        return [
            pltpu.make_async_copy(vout.at[at], vgrad_hbm.at[at], out_sem.at[0, c]),
            pltpu.make_async_copy(gout.at[at], ggrad_hbm.at[at], out_sem.at[1, c]),
        ]

    def grad_loop(c, carry):
        at = rows_of(c)
        base = c * BLOCK
        for h in range(halves):
            cols = slice(h * LANES, (h + 1) * LANES)
            grad = conv_block(cg, h, base, 0, lambda j: klen - 1 - j)
            sig = gsig[h, at, :]
            scaled = grad * sig
            vout[at, cols] = scaled.astype(BF16)
            gout[at, cols] = (scaled * value_v[at, cols].astype(F32) * (1.0 - sig)).astype(BF16)
        for copy in out_copies(c):
            copy.start()
        return carry

    lax.fori_loop(0, blocks - 1, grad_loop, 0)

    @pl.when(sp < n_sp - 1)
    def _():
        cg_copy.wait_recv()

    @pl.when(sp == n_sp - 1)
    def _():
        for h in range(halves):
            cg[h, pl.ds(rows, halo), :] = jnp.zeros((halo, LANES), F32)

    lax.fori_loop(blocks - 1, blocks, grad_loop, 0)

    if fused:
        taps_total = taps_sum
        for o in range(1, n_sp):
            tg_copy(o).wait_recv()
            taps_total = taps_total + tg_in[o - 1].astype(F32)
        taps_out[...] = taps_total
        for o in hops:
            rs_copy(o, pl.ds(0, out_cols)).wait_recv()
        proj = rs_own[sp]
        for o in hops:
            proj = proj + rs_in[o - 1].astype(F32)
        proj_out[...] = proj
        for o in hops:
            rs_copy(o, pl.ds(0, out_cols)).wait_send()
            tg_copy(o).wait_send()
    for copy in ex1 + ex2:
        copy.wait_send()

    @pl.when(sp < n_sp - 1)
    def _():
        for copy in halo_copies():
            copy.wait_send()

    @pl.when(sp > 0)
    def _():
        cg_copy.wait_send()

    def drain(c, carry):
        for copy in out_copies(c):
            copy.wait()
        return carry

    lax.fori_loop(0, blocks, drain, 0)


def per_device(glu_value, glu_gate, conv_taps, channel_gain, proj_weight, out_grad):
    rows, width = glu_value.shape
    klen = conv_taps.shape[0]
    out_cols = out_grad.shape[1]
    n_sp, n_tp = lax.axis_size("sp"), lax.axis_size("tp")
    halo = -(-(klen - 1) // 16) * 16
    own = width // n_sp
    fused = width % n_sp == 0 and own % 16 == 0
    halves = width // LANES
    blocks = rows // BLOCK
    peers = max(n_sp - 1, 1) if fused else 1
    cfg = (rows, width, klen, halo, n_sp, n_tp, fused)
    rs_shape = (n_sp, own, out_cols) if fused else (1, 16, out_cols)
    vm, dma = pltpu.VMEM, pltpu.SemaphoreType.DMA
    slots = max(n_tp - 1, 1)
    scratch = [
        vm((rows, width), BF16), vm((rows, width), BF16),
        vm((width, out_cols), BF16), vm((rows, out_cols), BF16),
        vm((halo, width), BF16), vm((halo, width), BF16),
        vm((halves, rows, LANES), F32),
        vm((halves, rows + halo, LANES), F32),
        vm((halves, rows, LANES), F32),
        vm((halves, rows + halo, LANES), F32),
        vm((width, rows), BF16),
        vm((klen, 8, width), F32), vm((klen + 1, 8, width), F32),
        vm((16, LANES), F32), vm((slots, 16, LANES), F32),
        vm((16, LANES), F32), vm((slots, 16, LANES), F32),
        vm(rs_shape, BF16), vm(rs_shape, F32), vm((peers,) + rs_shape[1:], BF16),
        vm((klen + 1, width), BF16), vm((peers, klen + 1, width), BF16),
        vm((rows, width), BF16), vm((rows, width), BF16),
        dma((4,)), dma((2, blocks)), dma((2,)), dma((2,)), dma, dma,
        dma((slots,)), dma((slots,)), dma((slots,)), dma((slots,)),
        dma((peers,)), dma((peers,)), dma((peers,)), dma((peers,)),
    ]
    anywhere = pl.BlockSpec(memory_space=pl.ANY)
    vmem = pl.BlockSpec(memory_space=pltpu.VMEM)
    proj_rows = own if fused else width
    value_grad, gate_grad, proj, taps = pl.pallas_call(
        functools.partial(kernel, cfg),
        out_shape=(
            jax.ShapeDtypeStruct((rows, width), BF16),
            jax.ShapeDtypeStruct((rows, width), BF16),
            jax.ShapeDtypeStruct((proj_rows, out_cols), F32),
            jax.ShapeDtypeStruct((klen + 1, width), F32),
        ),
        in_specs=[anywhere, anywhere, vmem, vmem, anywhere, anywhere],
        out_specs=(anywhere, anywhere, vmem, vmem),
        scratch_shapes=scratch,
        compiler_params=pltpu.CompilerParams(
            collective_id=0, has_side_effects=True, vmem_limit_bytes=60 * 1024 * 1024
        ),
    )(glu_value, glu_gate, conv_taps, channel_gain[None, :], proj_weight, out_grad)
    if not fused:
        proj = lax.psum_scatter(proj, "sp", scatter_dimension=0, tiled=True)
        taps = lax.psum(taps, "sp")
    return value_grad, gate_grad, proj, taps[:klen], taps[klen]


def solution(mesh):
    from jax.sharding import PartitionSpec as P

    return jax.shard_map(
        per_device,
        mesh=mesh,
        in_specs=(
            P("sp", "tp"),
            P("sp", "tp"),
            P(None, "tp"),
            P("tp"),
            P("tp", None),
            P("sp", None),
        ),
        out_specs=(P("sp", "tp"), P("sp", "tp"), P(("tp", "sp"), None), P(None, "tp"), P("tp")),
        check_vma=False,
    )
```

```python
import functools

import jax
import jax.numpy as jnp
from jax import lax
from jax.experimental import pallas as pl
from jax.experimental.pallas import tpu as pltpu

MESH = pl.DeviceIdType.MESH
F32 = jnp.float32
BF16 = jnp.bfloat16
LANES = 128
BLOCK = 128


def split_two(x):
    hi = x.astype(BF16)
    return hi, (x - hi.astype(F32)).astype(BF16)


def split_three(x):
    hi = x.astype(BF16).astype(F32)
    rest = x - hi
    mid = rest.astype(BF16).astype(F32)
    low = (rest - mid).astype(BF16).astype(F32)
    return [hi, mid, low]


def nt(a, b):
    return lax.dot_general(a, b, (((1,), (1,)), ((), ())), preferred_element_type=F32)


def nn(a, b):
    return lax.dot_general(a, b, (((1,), (0,)), ((), ())), preferred_element_type=F32)


def kernel(
    cfg,
    value_hbm, gate_hbm, taps_ref, gain_ref, weight_hbm, cot_hbm,
    vout, gout, proj_out, taps_out,
    value_v, gate_v, weight_v, cot_v, halo_v, halo_g, gsig, nsig, glu, xbuf, cg, act_t,
    taps_b, taps_acc, st1, st1_in, st2, st2_in, rs_send, rs_own, rs_in,
    tg_send, tg_in,
    in_sem, halo_send, halo_recv, cgs_send, cgs_recv,
    s1_send, s1_recv, s2_send, s2_recv, rs_ssem, rs_rsem, tg_ssem, tg_rsem,
):
    rows, width, klen, halo, n_sp, n_tp, fused = cfg
    halves = width // LANES
    blocks = rows // BLOCK
    channels = width * n_tp
    lead = halo - (klen - 1)
    factor = 1.0 / jnp.sqrt(F32(rows * n_sp))
    sp = lax.axis_index("sp")
    tp = lax.axis_index("tp")

    loads = [
        pltpu.make_async_copy(src, dst, in_sem.at[i])
        for i, (src, dst) in enumerate(
            [(value_hbm, value_v), (gate_hbm, gate_v), (weight_hbm, weight_v), (cot_hbm, cot_v)]
        )
    ]
    for copy in loads:
        copy.start()

    barrier = pltpu.get_barrier_semaphore()
    sp_hops = list(range(1, n_sp)) if fused else [1, n_sp - 1]
    for o in sp_hops:
        pl.semaphore_signal(
            barrier, inc=1, device_id=(lax.rem(sp + o, n_sp), tp), device_id_type=MESH
        )
    for o in range(1, n_tp):
        pl.semaphore_signal(
            barrier, inc=1, device_id=(sp, lax.rem(tp + o, n_tp)), device_id_type=MESH
        )

    for k in range(klen):
        taps_b[k] = jnp.broadcast_to(taps_ref[k : k + 1, :], (8, width))
    taps_acc[...] = jnp.zeros_like(taps_acc)
    st1[...] = jnp.zeros_like(st1)
    st2[...] = jnp.zeros_like(st2)

    loads[0].wait()
    loads[1].wait()
    nxt = (jnp.minimum(sp + 1, n_sp - 1), tp)
    prv = (jnp.maximum(sp - 1, 0), tp)

    def halo_copies():
        tail = pl.ds(rows - halo, halo)
        return [
            pltpu.make_async_remote_copy(
                src_ref=src.at[tail], dst_ref=dst, send_sem=halo_send.at[i],
                recv_sem=halo_recv.at[i], device_id=nxt, device_id_type=MESH,
            )
            for i, (src, dst) in enumerate([(value_v, halo_v), (gate_v, halo_g)])
        ]

    def rows_of(c):
        return pl.ds(pl.multiple_of(c * BLOCK, BLOCK), BLOCK)

    def glu_block(c, carry):
        at = rows_of(c)
        to = pl.ds(pl.multiple_of(c * BLOCK + halo, 8), BLOCK)
        sig = jax.nn.sigmoid(gate_v[at, :].astype(F32))
        out = value_v[at, :].astype(F32) * sig
        for h in range(halves):
            cols = slice(h * LANES, (h + 1) * LANES)
            gsig[h, at, :] = sig[:, cols]
            glu[h, to, :] = out[:, cols]
        return carry

    lax.fori_loop(0, blocks, glu_block, 0)
    pl.semaphore_wait(barrier, len(sp_hops) + n_tp - 1)

    @pl.when(sp < n_sp - 1)
    def _():
        for copy in halo_copies():
            copy.start()

    def conv_block(src, h, base, first, tap_of):
        cols = slice(h * LANES, (h + 1) * LANES)
        acc = None
        for s in range(8):
            qs = [q for q in range((first + klen + 7) // 8 + 1) if first <= 8 * q + s < first + klen]
            if not qs:
                continue
            lo = qs[0]
            span = BLOCK + 8 * (qs[-1] - lo)
            slab = src[h, pl.ds(base + (8 * lo + s), span), :]
            for q in qs:
                tap = taps_b[tap_of(8 * q + s - first), :, cols]
                part = slab[8 * (q - lo) : 8 * (q - lo) + BLOCK]
                term = part.reshape(BLOCK // 8, 8, LANES) * tap[None]
                acc = term if acc is None else acc + term
        return acc.reshape(BLOCK, LANES)

    def place_sums(ref, c, first, second):
        which = lax.broadcasted_iota(jnp.int32, (16, width), 0)
        one = jnp.where(which == c, 1.0, 0.0).astype(BF16)
        two = jnp.where(which == c + 8, 1.0, 0.0).astype(BF16)
        total = ref[...]
        for sel, x in ((one, first), (two, second)):
            hi, low = split_two(x)
            total = total + nt(sel, hi) + nt(sel, low)
        ref[...] = total

    def forward_block(c):
        base = c * BLOCK
        at = rows_of(c)
        parts = []
        for h in range(halves):
            out = conv_block(glu, h, base, lead, lambda k: k)
            xbuf[h, at, :] = out
            parts.append(out)
        x = jnp.concatenate(parts, axis=1)
        place_sums(st1, c, x, x * x)

    def fwd_loop(c, carry):
        forward_block(c)
        return carry

    lax.fori_loop(1, blocks, fwd_loop, 0)

    @pl.when(sp > 0)
    def _():
        for copy in halo_copies():
            copy.wait_recv()
        out = halo_v[...].astype(F32) * jax.nn.sigmoid(halo_g[...].astype(F32))
        for h in range(halves):
            glu[h, 0:halo, :] = out[:, h * LANES : (h + 1) * LANES]

    @pl.when(sp == 0)
    def _():
        for h in range(halves):
            glu[h, 0:halo, :] = jnp.zeros((halo, LANES), F32)

    lax.fori_loop(0, 1, fwd_loop, 0)

    def tp_copies(src, dst, ssem, rsem):
        return [
            pltpu.make_async_remote_copy(
                src_ref=src, dst_ref=dst.at[o - 1], send_sem=ssem.at[o - 1],
                recv_sem=rsem.at[o - 1], device_id=(sp, lax.rem(tp + o, n_tp)),
                device_id_type=MESH,
            )
            for o in range(1, n_tp)
        ]

    ex1 = tp_copies(st1, st1_in, s1_send, s1_recv)
    for copy in ex1:
        copy.start()
    loads[2].wait()
    loads[3].wait()

    def act_grad_block(c, carry):
        at = rows_of(c)
        out = nt(cot_v[at, :], weight_v[...])
        for h in range(halves):
            cg[h, at, :] = out[:, h * LANES : (h + 1) * LANES]
        return carry

    lax.fori_loop(0, blocks, act_grad_block, 0)
    for copy in ex1:
        copy.wait_recv()

    total = st1[...]
    for o in range(n_tp - 1):
        total = total + st1_in[o]
    mean = total[0:8] / channels
    rstd = lax.rsqrt(total[8:16] / channels - mean * mean + 1e-05)

    def columns(a, b):
        stack = split_three(a) + split_three(b)
        stack.append(jnp.zeros((LANES - 48, LANES), F32))
        return jnp.transpose(jnp.concatenate(stack, axis=0)).astype(BF16)

    def spread(cols, c):
        k = lax.broadcasted_iota(jnp.int32, (LANES, 2 * LANES), 0)
        j = lax.broadcasted_iota(jnp.int32, (LANES, 2 * LANES), 1)
        low = jnp.where(j < LANES, 0, 24)
        hit = (k == c + low) | (k == c + low + 8) | (k == c + low + 16)
        out = nn(cols, jnp.where(hit, 1.0, 0.0).astype(BF16))
        return out[:, :LANES], out[:, LANES:]

    cols1 = columns(mean, rstd)

    def activ_block(c, carry):
        at = rows_of(c)
        mean_b, rstd_b = spread(cols1, c)
        activs = []
        for h in range(halves):
            cols = slice(h * LANES, (h + 1) * LANES)
            xhat = (xbuf[h, at, :] - mean_b) * rstd_b
            normed = xhat * gain_ref[0:1, cols]
            sig = jax.nn.sigmoid(normed)
            xbuf[h, at, :] = xhat
            nsig[h, at, :] = sig
            activs.append(normed * sig)
        act_t[:, at] = jnp.transpose(jnp.concatenate(activs, axis=1)).astype(BF16)
        return carry

    lax.fori_loop(0, blocks, activ_block, 0)

    out_cols = proj_out.shape[-1]
    tile = 256
    hops = list(range(1, n_sp)) if fused else []
    hops.sort(key=lambda o: -min(o, n_sp - o))

    def rs_copy(o, cols):
        dest = lax.rem(sp + o, n_sp)
        return pltpu.make_async_remote_copy(
            src_ref=rs_send.at[dest, :, cols], dst_ref=rs_in.at[o - 1, :, cols],
            send_sem=rs_ssem.at[o - 1], recv_sem=rs_rsem.at[o - 1],
            device_id=(dest, tp), device_id_type=MESH,
        )

    for nb in range(out_cols // tile):
        cols = slice(nb * tile, (nb + 1) * tile)
        part = nn(act_t[...], cot_v[:, cols]) * factor
        if fused:
            own = width // n_sp
            rs_own[:, :, cols] = part.reshape(n_sp, own, tile)
            rs_send[:, :, cols] = part.astype(BF16).reshape(n_sp, own, tile)
            for o in hops:
                rs_copy(o, pl.ds(nb * tile, tile)).start()
        else:
            proj_out[:, cols] = part

    def norm_block(c, carry):
        at = rows_of(c)
        firsts, seconds = [], []
        for h in range(halves):
            cols = slice(h * LANES, (h + 1) * LANES)
            gain = gain_ref[0:1, cols]
            xhat = xbuf[h, at, :]
            sig = nsig[h, at, :]
            ngrad = cg[h, at, :] * sig * (1.0 + xhat * gain * (1.0 - sig))
            xgrad = ngrad * gain
            taps_acc[klen, :, cols] += jnp.sum(
                (ngrad * xhat).reshape(BLOCK // 8, 8, LANES), axis=0
            )
            cg[h, at, :] = xgrad
            firsts.append(xgrad)
            seconds.append(xgrad * xhat)
        place_sums(st2, c, jnp.concatenate(firsts, axis=1), jnp.concatenate(seconds, axis=1))
        return carry

    lax.fori_loop(0, blocks, norm_block, 0)

    ex2 = tp_copies(st2, st2_in, s2_send, s2_recv)
    for copy in ex2:
        copy.start()
    for copy in ex2:
        copy.wait_recv()
    total = st2[...]
    for o in range(n_tp - 1):
        total = total + st2_in[o]
    cols2 = columns(total[0:8] / channels, total[8:16] / channels)

    def cgrad_block(c):
        at = rows_of(c)
        base = c * BLOCK
        _, rstd_b = spread(cols1, c)
        one_b, two_b = spread(cols2, c)
        for h in range(halves):
            cols = slice(h * LANES, (h + 1) * LANES)
            grad = rstd_b * (cg[h, at, :] - one_b - xbuf[h, at, :] * two_b)
            cg[h, at, :] = grad
            grad3 = grad.reshape(BLOCK // 8, 8, LANES)
            for s in range(8):
                qs = [q for q in range((lead + klen + 7) // 8 + 1) if lead <= 8 * q + s < lead + klen]
                if not qs:
                    continue
                lo = qs[0]
                span = BLOCK + 8 * (qs[-1] - lo)
                slab = glu[h, pl.ds(base + (8 * lo + s), span), :]
                for q in qs:
                    part = slab[8 * (q - lo) : 8 * (q - lo) + BLOCK]
                    prod = grad3 * part.reshape(BLOCK // 8, 8, LANES)
                    taps_acc[8 * q + s - lead, :, cols] += jnp.sum(prod, axis=0)

    def cgrad_loop(c, carry):
        cgrad_block(c)
        return carry

    lax.fori_loop(0, 1, cgrad_loop, 0)

    cg_copy = pltpu.make_async_remote_copy(
        src_ref=cg.at[:, pl.ds(0, halo), :], dst_ref=cg.at[:, pl.ds(rows, halo), :],
        send_sem=cgs_send, recv_sem=cgs_recv, device_id=prv, device_id_type=MESH,
    )

    @pl.when(sp > 0)
    def _():
        cg_copy.start()

    lax.fori_loop(1, blocks, cgrad_loop, 0)

    taps_sum = jnp.sum(taps_acc[...], axis=1) * factor
    taps_out[...] = taps_sum

    def tg_copy(o):
        return pltpu.make_async_remote_copy(
            src_ref=tg_send, dst_ref=tg_in.at[o - 1],
            send_sem=tg_ssem.at[o - 1], recv_sem=tg_rsem.at[o - 1],
            device_id=(lax.rem(sp + o, n_sp), tp), device_id_type=MESH,
        )

    if fused:
        tg_send[...] = taps_sum.astype(BF16)
        for o in hops:
            tg_copy(o).start()

    def grad_loop(c, carry):
        at = rows_of(c)
        base = c * BLOCK
        for h in range(halves):
            cols = slice(h * LANES, (h + 1) * LANES)
            grad = conv_block(cg, h, base, 0, lambda j: klen - 1 - j)
            sig = gsig[h, at, :]
            scaled = grad * sig
            vout[at, cols] = scaled.astype(BF16)
            gout[at, cols] = (scaled * value_v[at, cols].astype(F32) * (1.0 - sig)).astype(BF16)
        return carry

    lax.fori_loop(0, blocks - 1, grad_loop, 0)

    @pl.when(sp < n_sp - 1)
    def _():
        cg_copy.wait_recv()

    @pl.when(sp == n_sp - 1)
    def _():
        for h in range(halves):
            cg[h, pl.ds(rows, halo), :] = jnp.zeros((halo, LANES), F32)

    lax.fori_loop(blocks - 1, blocks, grad_loop, 0)

    if fused:
        taps_total = taps_sum
        for o in range(1, n_sp):
            tg_copy(o).wait_recv()
            taps_total = taps_total + tg_in[o - 1].astype(F32)
        taps_out[...] = taps_total
        for o in hops:
            rs_copy(o, pl.ds(0, out_cols)).wait_recv()
        proj = rs_own[sp]
        for o in hops:
            proj = proj + rs_in[o - 1].astype(F32)
        proj_out[...] = proj
        for o in hops:
            rs_copy(o, pl.ds(0, out_cols)).wait_send()
            tg_copy(o).wait_send()
    for copy in ex1 + ex2:
        copy.wait_send()

    @pl.when(sp < n_sp - 1)
    def _():
        for copy in halo_copies():
            copy.wait_send()

    @pl.when(sp > 0)
    def _():
        cg_copy.wait_send()


def finish_kernel(
    value_ref, gate_ref, proj_ref, taps_ref, value_out, gate_out, proj_out, taps_out, gain_out, sem
):
    pairs = [(value_ref, value_out), (gate_ref, gate_out), (proj_ref, proj_out)]
    copies = [pltpu.make_async_copy(a, b, sem.at[i]) for i, (a, b) in enumerate(pairs)]
    for copy in copies:
        copy.start()
    klen = taps_out.shape[0]
    taps_out[...] = taps_ref[0:klen, :]
    gain_out[...] = taps_ref[klen : klen + 1, :]
    for copy in copies:
        copy.wait()


def per_device(glu_value, glu_gate, conv_taps, channel_gain, proj_weight, out_grad):
    rows, width = glu_value.shape
    klen = conv_taps.shape[0]
    out_cols = out_grad.shape[1]
    n_sp, n_tp = lax.axis_size("sp"), lax.axis_size("tp")
    halo = -(-(klen - 1) // 16) * 16
    own = width // n_sp
    fused = width % n_sp == 0 and own % 16 == 0
    halves = width // LANES
    blocks = rows // BLOCK
    peers = max(n_sp - 1, 1) if fused else 1
    cfg = (rows, width, klen, halo, n_sp, n_tp, fused)
    rs_shape = (n_sp, own, out_cols) if fused else (1, 16, out_cols)
    vm, dma = pltpu.VMEM, pltpu.SemaphoreType.DMA
    slots = max(n_tp - 1, 1)
    scratch = [
        vm((rows, width), BF16), vm((rows, width), BF16),
        vm((width, out_cols), BF16), vm((rows, out_cols), BF16),
        vm((halo, width), BF16), vm((halo, width), BF16),
        vm((halves, rows, LANES), F32), vm((halves, rows, LANES), F32),
        vm((halves, rows + halo, LANES), F32),
        vm((halves, rows, LANES), F32),
        vm((halves, rows + halo, LANES), F32),
        vm((width, rows), BF16),
        vm((klen, 8, width), F32), vm((klen + 1, 8, width), F32),
        vm((16, LANES), F32), vm((slots, 16, LANES), F32),
        vm((16, LANES), F32), vm((slots, 16, LANES), F32),
        vm(rs_shape, BF16), vm(rs_shape, F32), vm((peers,) + rs_shape[1:], BF16),
        vm((klen + 1, width), BF16), vm((peers, klen + 1, width), BF16),
        dma((4,)), dma((2,)), dma((2,)), dma, dma,
        dma((slots,)), dma((slots,)), dma((slots,)), dma((slots,)),
        dma((peers,)), dma((peers,)), dma((peers,)), dma((peers,)),
    ]
    hbm = pl.BlockSpec(memory_space=pltpu.HBM)
    vmem = pl.BlockSpec(memory_space=pltpu.VMEM)
    proj_rows = own if fused else width
    out_bytes = 4 * (rows * width + proj_rows * out_cols + (klen + 1) * width)
    value_grad, gate_grad, proj, taps = pl.pallas_call(
        functools.partial(kernel, cfg),
        out_shape=(
            pltpu.VMEM((rows, width), BF16),
            pltpu.VMEM((rows, width), BF16),
            pltpu.VMEM((proj_rows, out_cols), F32),
            pltpu.VMEM((klen + 1, width), F32),
        ),
        in_specs=[hbm, hbm, vmem, vmem, hbm, hbm],
        out_specs=(vmem, vmem, vmem, vmem),
        scratch_shapes=scratch,
        compiler_params=pltpu.CompilerParams(
            collective_id=0, has_side_effects=True, vmem_limit_bytes=65 * 1024 * 1000 - out_bytes
        ),
    )(glu_value, glu_gate, conv_taps, channel_gain[None, :], proj_weight, out_grad)
    if not fused:
        proj = lax.psum_scatter(proj, "sp", scatter_dimension=0, tiled=True)
        taps = lax.psum(taps, "sp")
    value_grad, gate_grad, proj, taps_grad, gain_grad = pl.pallas_call(
        finish_kernel,
        out_shape=(
            jax.ShapeDtypeStruct((rows, width), BF16),
            jax.ShapeDtypeStruct((rows, width), BF16),
            jax.ShapeDtypeStruct(proj.shape, F32),
            jax.ShapeDtypeStruct((klen, width), F32),
            jax.ShapeDtypeStruct((1, width), F32),
        ),
        in_specs=[vmem] * 4,
        out_specs=(hbm, hbm, hbm, vmem, vmem),
        scratch_shapes=[dma((3,))],
        compiler_params=pltpu.CompilerParams(vmem_limit_bytes=8 * 1024 * 1024),
    )(value_grad, gate_grad, proj, taps)
    return value_grad, gate_grad, proj, taps_grad, gain_grad[0]


def solution(mesh):
    from jax.sharding import PartitionSpec as P

    return jax.shard_map(
        per_device,
        mesh=mesh,
        in_specs=(
            P("sp", "tp"),
            P("sp", "tp"),
            P(None, "tp"),
            P("tp"),
            P("tp", None),
            P("sp", None),
        ),
        out_specs=(P("sp", "tp"), P("sp", "tp"), P(("tp", "sp"), None), P(None, "tp"), P("tp")),
        check_vma=False,
    )
```

```python
import functools

import jax
import jax.numpy as jnp
from jax import lax
from jax.experimental import pallas as pl
from jax.experimental.pallas import tpu as pltpu

MESH = pl.DeviceIdType.MESH
F32 = jnp.float32
BF16 = jnp.bfloat16
LANES = 128
BLOCK = 128


def split_two(x):
    hi = x.astype(BF16)
    return hi, (x - hi.astype(F32)).astype(BF16)


def split_three(x):
    hi = x.astype(BF16).astype(F32)
    rest = x - hi
    mid = rest.astype(BF16).astype(F32)
    low = (rest - mid).astype(BF16).astype(F32)
    return [hi, mid, low]


def nt(a, b):
    return lax.dot_general(a, b, (((1,), (1,)), ((), ())), preferred_element_type=F32)


def nn(a, b):
    return lax.dot_general(a, b, (((1,), (0,)), ((), ())), preferred_element_type=F32)


def kernel(
    cfg,
    value_hbm, gate_hbm, taps_hbm, gain_hbm, weight_hbm, cot_hbm,
    vout, gout, proj_out, taps_out,
    taps_ref, gain_ref, value_v, gate_v, weight_v, cot_v, halo_v, halo_g, gsig, nsig, glu, xbuf, cg, act_t,
    taps_b, taps_acc, st1, st1_in, st2, st2_in, rs_send, rs_own, rs_in,
    tg_send, tg_in,
    in_sem, halo_send, halo_recv, cgs_send, cgs_recv,
    s1_send, s1_recv, s2_send, s2_recv, rs_ssem, rs_rsem, tg_ssem, tg_rsem,
):
    rows, width, klen, halo, n_sp, n_tp, fused = cfg
    halves = width // LANES
    blocks = rows // BLOCK
    channels = width * n_tp
    lead = halo - (klen - 1)
    factor = 1.0 / jnp.sqrt(F32(rows * n_sp))
    sp = lax.axis_index("sp")
    tp = lax.axis_index("tp")

    loads = [
        pltpu.make_async_copy(src, dst, in_sem.at[i])
        for i, (src, dst) in enumerate(
            [
                (value_hbm, value_v), (gate_hbm, gate_v), (weight_hbm, weight_v),
                (cot_hbm, cot_v), (taps_hbm, taps_ref), (gain_hbm, gain_ref),
            ]
        )
    ]
    for i in (0, 1, 4, 5, 2, 3):
        loads[i].start()
    barrier = pltpu.get_barrier_semaphore()
    sp_hops = list(range(1, n_sp)) if fused else [1, n_sp - 1]
    for o in sp_hops:
        pl.semaphore_signal(
            barrier, inc=1, device_id=(lax.rem(sp + o, n_sp), tp), device_id_type=MESH
        )
    for o in range(1, n_tp):
        pl.semaphore_signal(
            barrier, inc=1, device_id=(sp, lax.rem(tp + o, n_tp)), device_id_type=MESH
        )

    taps_acc[...] = jnp.zeros_like(taps_acc)
    st1[...] = jnp.zeros_like(st1)
    st2[...] = jnp.zeros_like(st2)

    loads[0].wait()
    loads[1].wait()
    nxt = (jnp.minimum(sp + 1, n_sp - 1), tp)
    prv = (jnp.maximum(sp - 1, 0), tp)

    def halo_copies():
        tail = pl.ds(rows - halo, halo)
        return [
            pltpu.make_async_remote_copy(
                src_ref=src.at[tail], dst_ref=dst, send_sem=halo_send.at[i],
                recv_sem=halo_recv.at[i], device_id=nxt, device_id_type=MESH,
            )
            for i, (src, dst) in enumerate([(value_v, halo_v), (gate_v, halo_g)])
        ]

    def rows_of(c):
        return pl.ds(pl.multiple_of(c * BLOCK, BLOCK), BLOCK)

    def glu_block(c, carry):
        at = rows_of(c)
        to = pl.ds(pl.multiple_of(c * BLOCK + halo, 8), BLOCK)
        sig = jax.nn.sigmoid(gate_v[at, :].astype(F32))
        out = value_v[at, :].astype(F32) * sig
        for h in range(halves):
            cols = slice(h * LANES, (h + 1) * LANES)
            gsig[h, at, :] = sig[:, cols]
            glu[h, to, :] = out[:, cols]
        return carry

    lax.fori_loop(0, blocks, glu_block, 0)
    loads[4].wait()
    loads[5].wait()
    for k in range(klen):
        taps_b[k] = jnp.broadcast_to(taps_ref[k : k + 1, :], (8, width))
    pl.semaphore_wait(barrier, len(sp_hops) + n_tp - 1)

    @pl.when(sp < n_sp - 1)
    def _():
        for copy in halo_copies():
            copy.start()

    def conv_block(src, h, base, first, tap_of):
        cols = slice(h * LANES, (h + 1) * LANES)
        acc = None
        for s in range(8):
            qs = [q for q in range((first + klen + 7) // 8 + 1) if first <= 8 * q + s < first + klen]
            if not qs:
                continue
            lo = qs[0]
            span = BLOCK + 8 * (qs[-1] - lo)
            slab = src[h, pl.ds(base + (8 * lo + s), span), :]
            for q in qs:
                tap = taps_b[tap_of(8 * q + s - first), :, cols]
                part = slab[8 * (q - lo) : 8 * (q - lo) + BLOCK]
                term = part.reshape(BLOCK // 8, 8, LANES) * tap[None]
                acc = term if acc is None else acc + term
        return acc.reshape(BLOCK, LANES)

    def place_sums(ref, c, first, second):
        which = lax.broadcasted_iota(jnp.int32, (16, width), 0)
        one = jnp.where(which == c, 1.0, 0.0).astype(BF16)
        two = jnp.where(which == c + 8, 1.0, 0.0).astype(BF16)
        total = ref[...]
        for sel, x in ((one, first), (two, second)):
            hi, low = split_two(x)
            total = total + nt(sel, hi) + nt(sel, low)
        ref[...] = total

    def forward_block(c):
        base = c * BLOCK
        at = rows_of(c)
        parts = []
        for h in range(halves):
            out = conv_block(glu, h, base, lead, lambda k: k)
            xbuf[h, at, :] = out
            parts.append(out)
        x = jnp.concatenate(parts, axis=1)
        place_sums(st1, c, x, x * x)

    def fwd_loop(i, carry):
        @pl.when((i == blocks - 1) & (sp > 0))
        def _():
            for copy in halo_copies():
                copy.wait_recv()
            out = halo_v[...].astype(F32) * jax.nn.sigmoid(halo_g[...].astype(F32))
            for h in range(halves):
                glu[h, 0:halo, :] = out[:, h * LANES : (h + 1) * LANES]

        @pl.when((i == blocks - 1) & (sp == 0))
        def _():
            for h in range(halves):
                glu[h, 0:halo, :] = jnp.zeros((halo, LANES), F32)

        forward_block(lax.rem(i + 1, blocks))
        return carry

    lax.fori_loop(0, blocks, fwd_loop, 0)

    def tp_copies(src, dst, ssem, rsem):
        return [
            pltpu.make_async_remote_copy(
                src_ref=src, dst_ref=dst.at[o - 1], send_sem=ssem.at[o - 1],
                recv_sem=rsem.at[o - 1], device_id=(sp, lax.rem(tp + o, n_tp)),
                device_id_type=MESH,
            )
            for o in range(1, n_tp)
        ]

    ex1 = tp_copies(st1, st1_in, s1_send, s1_recv)
    for copy in ex1:
        copy.start()
    loads[2].wait()
    loads[3].wait()

    def act_grad_block(c, carry):
        at = rows_of(c)
        out = nt(cot_v[at, :], weight_v[...])
        for h in range(halves):
            cg[h, at, :] = out[:, h * LANES : (h + 1) * LANES]
        return carry

    lax.fori_loop(0, blocks, act_grad_block, 0)
    for copy in ex1:
        copy.wait_recv()

    total = st1[...]
    for o in range(n_tp - 1):
        total = total + st1_in[o]
    mean = total[0:8] / channels
    rstd = lax.rsqrt(total[8:16] / channels - mean * mean + 1e-05)

    def columns(a, b):
        stack = split_three(a) + split_three(b)
        stack.append(jnp.zeros((LANES - 48, LANES), F32))
        return jnp.transpose(jnp.concatenate(stack, axis=0)).astype(BF16)

    def spread(cols, c):
        k = lax.broadcasted_iota(jnp.int32, (LANES, 2 * LANES), 0)
        j = lax.broadcasted_iota(jnp.int32, (LANES, 2 * LANES), 1)
        low = jnp.where(j < LANES, 0, 24)
        hit = (k == c + low) | (k == c + low + 8) | (k == c + low + 16)
        out = nn(cols, jnp.where(hit, 1.0, 0.0).astype(BF16))
        return out[:, :LANES], out[:, LANES:]

    cols1 = columns(mean, rstd)

    def activ_block(c, carry):
        at = rows_of(c)
        mean_b, rstd_b = spread(cols1, c)
        activs = []
        for h in range(halves):
            cols = slice(h * LANES, (h + 1) * LANES)
            xhat = (xbuf[h, at, :] - mean_b) * rstd_b
            normed = xhat * gain_ref[0:1, cols]
            sig = jax.nn.sigmoid(normed)
            xbuf[h, at, :] = xhat
            nsig[h, at, :] = sig
            activs.append(normed * sig)
        act_t[:, at] = jnp.transpose(jnp.concatenate(activs, axis=1)).astype(BF16)
        return carry

    lax.fori_loop(0, blocks, activ_block, 0)

    out_cols = proj_out.shape[-1]
    tile = 256
    hops = list(range(1, n_sp)) if fused else []
    hops.sort(key=lambda o: -min(o, n_sp - o))

    def rs_copy(o, cols):
        dest = lax.rem(sp + o, n_sp)
        return pltpu.make_async_remote_copy(
            src_ref=rs_send.at[dest, :, cols], dst_ref=rs_in.at[o - 1, :, cols],
            send_sem=rs_ssem.at[o - 1], recv_sem=rs_rsem.at[o - 1],
            device_id=(dest, tp), device_id_type=MESH,
        )

    for nb in range(out_cols // tile):
        cols = slice(nb * tile, (nb + 1) * tile)
        part = nn(act_t[...], cot_v[:, cols]) * factor
        if fused:
            own = width // n_sp
            rs_own[:, :, cols] = part.reshape(n_sp, own, tile)
            rs_send[:, :, cols] = part.astype(BF16).reshape(n_sp, own, tile)
            for o in hops:
                rs_copy(o, pl.ds(nb * tile, tile)).start()
        else:
            proj_out[:, cols] = part

    def norm_block(c, carry):
        at = rows_of(c)
        firsts, seconds = [], []
        for h in range(halves):
            cols = slice(h * LANES, (h + 1) * LANES)
            gain = gain_ref[0:1, cols]
            xhat = xbuf[h, at, :]
            sig = nsig[h, at, :]
            ngrad = cg[h, at, :] * sig * (1.0 + xhat * gain * (1.0 - sig))
            xgrad = ngrad * gain
            taps_acc[klen, :, cols] += jnp.sum(
                (ngrad * xhat).reshape(BLOCK // 8, 8, LANES), axis=0
            )
            cg[h, at, :] = xgrad
            firsts.append(xgrad)
            seconds.append(xgrad * xhat)
        place_sums(st2, c, jnp.concatenate(firsts, axis=1), jnp.concatenate(seconds, axis=1))
        return carry

    lax.fori_loop(0, blocks, norm_block, 0)

    ex2 = tp_copies(st2, st2_in, s2_send, s2_recv)
    for copy in ex2:
        copy.start()
    for copy in ex2:
        copy.wait_recv()
    total = st2[...]
    for o in range(n_tp - 1):
        total = total + st2_in[o]
    cols2 = columns(total[0:8] / channels, total[8:16] / channels)

    def cgrad_block(c):
        at = rows_of(c)
        base = c * BLOCK
        _, rstd_b = spread(cols1, c)
        one_b, two_b = spread(cols2, c)
        for h in range(halves):
            cols = slice(h * LANES, (h + 1) * LANES)
            grad = rstd_b * (cg[h, at, :] - one_b - xbuf[h, at, :] * two_b)
            cg[h, at, :] = grad
            grad3 = grad.reshape(BLOCK // 8, 8, LANES)
            for s in range(8):
                qs = [q for q in range((lead + klen + 7) // 8 + 1) if lead <= 8 * q + s < lead + klen]
                if not qs:
                    continue
                lo = qs[0]
                span = BLOCK + 8 * (qs[-1] - lo)
                slab = glu[h, pl.ds(base + (8 * lo + s), span), :]
                for q in qs:
                    part = slab[8 * (q - lo) : 8 * (q - lo) + BLOCK]
                    prod = grad3 * part.reshape(BLOCK // 8, 8, LANES)
                    taps_acc[8 * q + s - lead, :, cols] += jnp.sum(prod, axis=0)

    def cgrad_loop(c, carry):
        cgrad_block(c)

        @pl.when((c == 0) & (sp > 0))
        def _():
            cg_copy.start()

        return carry

    cg_copy = pltpu.make_async_remote_copy(
        src_ref=cg.at[:, pl.ds(0, halo), :], dst_ref=cg.at[:, pl.ds(rows, halo), :],
        send_sem=cgs_send, recv_sem=cgs_recv, device_id=prv, device_id_type=MESH,
    )

    lax.fori_loop(0, blocks, cgrad_loop, 0)

    taps_sum = jnp.sum(taps_acc[...], axis=1) * factor
    taps_out[...] = taps_sum

    def tg_copy(o):
        return pltpu.make_async_remote_copy(
            src_ref=tg_send, dst_ref=tg_in.at[o - 1],
            send_sem=tg_ssem.at[o - 1], recv_sem=tg_rsem.at[o - 1],
            device_id=(lax.rem(sp + o, n_sp), tp), device_id_type=MESH,
        )

    if fused:
        tg_send[...] = taps_sum.astype(BF16)
        for o in hops:
            tg_copy(o).start()

    def grad_loop(c, carry):
        @pl.when((c == blocks - 1) & (sp < n_sp - 1))
        def _():
            cg_copy.wait_recv()

        @pl.when((c == blocks - 1) & (sp == n_sp - 1))
        def _():
            for h in range(halves):
                cg[h, pl.ds(rows, halo), :] = jnp.zeros((halo, LANES), F32)

        at = rows_of(c)
        base = c * BLOCK
        for h in range(halves):
            cols = slice(h * LANES, (h + 1) * LANES)
            grad = conv_block(cg, h, base, 0, lambda j: klen - 1 - j)
            sig = gsig[h, at, :]
            scaled = grad * sig
            vout[at, cols] = scaled.astype(BF16)
            gout[at, cols] = (scaled * value_v[at, cols].astype(F32) * (1.0 - sig)).astype(BF16)
        return carry

    lax.fori_loop(0, blocks, grad_loop, 0)

    if fused:
        taps_total = taps_sum
        for o in range(1, n_sp):
            tg_copy(o).wait_recv()
            taps_total = taps_total + tg_in[o - 1].astype(F32)
        taps_out[...] = taps_total
        for o in hops:
            rs_copy(o, pl.ds(0, out_cols)).wait_recv()
        proj = rs_own[sp]
        for o in hops:
            proj = proj + rs_in[o - 1].astype(F32)
        proj_out[...] = proj
        for o in hops:
            rs_copy(o, pl.ds(0, out_cols)).wait_send()
            tg_copy(o).wait_send()
    for copy in ex1 + ex2:
        copy.wait_send()

    @pl.when(sp < n_sp - 1)
    def _():
        for copy in halo_copies():
            copy.wait_send()

    @pl.when(sp > 0)
    def _():
        cg_copy.wait_send()


def finish_kernel(
    value_ref, gate_ref, proj_ref, taps_ref, value_out, gate_out, proj_out, taps_out, gain_out, sem
):
    pairs = [(value_ref, value_out), (gate_ref, gate_out), (proj_ref, proj_out)]
    copies = [pltpu.make_async_copy(a, b, sem.at[i]) for i, (a, b) in enumerate(pairs)]
    for copy in copies:
        copy.start()
    klen = taps_out.shape[0]
    taps_out[...] = taps_ref[0:klen, :]
    gain_out[...] = taps_ref[klen : klen + 1, :]
    for copy in copies:
        copy.wait()


def per_device(glu_value, glu_gate, conv_taps, channel_gain, proj_weight, out_grad):
    rows, width = glu_value.shape
    klen = conv_taps.shape[0]
    out_cols = out_grad.shape[1]
    n_sp, n_tp = lax.axis_size("sp"), lax.axis_size("tp")
    halo = -(-(klen - 1) // 16) * 16
    own = width // n_sp
    fused = width % n_sp == 0 and own % 16 == 0
    halves = width // LANES
    blocks = rows // BLOCK
    peers = max(n_sp - 1, 1) if fused else 1
    cfg = (rows, width, klen, halo, n_sp, n_tp, fused)
    rs_shape = (n_sp, own, out_cols) if fused else (1, 16, out_cols)
    vm, dma = pltpu.VMEM, pltpu.SemaphoreType.DMA
    slots = max(n_tp - 1, 1)
    scratch = [
        vm((klen, width), F32), vm((1, width), F32),
        vm((rows, width), BF16), vm((rows, width), BF16),
        vm((width, out_cols), BF16), vm((rows, out_cols), BF16),
        vm((halo, width), BF16), vm((halo, width), BF16),
        vm((halves, rows, LANES), F32), vm((halves, rows, LANES), F32),
        vm((halves, rows + halo, LANES), F32),
        vm((halves, rows, LANES), F32),
        vm((halves, rows + halo, LANES), F32),
        vm((width, rows), BF16),
        vm((klen, 8, width), F32), vm((klen + 1, 8, width), F32),
        vm((16, LANES), F32), vm((slots, 16, LANES), F32),
        vm((16, LANES), F32), vm((slots, 16, LANES), F32),
        vm(rs_shape, BF16), vm(rs_shape, F32), vm((peers,) + rs_shape[1:], BF16),
        vm((klen + 1, width), BF16), vm((peers, klen + 1, width), BF16),
        dma((6,)), dma((2,)), dma((2,)), dma, dma,
        dma((slots,)), dma((slots,)), dma((slots,)), dma((slots,)),
        dma((peers,)), dma((peers,)), dma((peers,)), dma((peers,)),
    ]
    hbm = pl.BlockSpec(memory_space=pltpu.HBM)
    vmem = pl.BlockSpec(memory_space=pltpu.VMEM)
    proj_rows = own if fused else width
    out_bytes = 4 * (rows * width + proj_rows * out_cols + (klen + 1) * width)
    value_grad, gate_grad, proj, taps = pl.pallas_call(
        functools.partial(kernel, cfg),
        out_shape=(
            pltpu.VMEM((rows, width), BF16),
            pltpu.VMEM((rows, width), BF16),
            pltpu.VMEM((proj_rows, out_cols), F32),
            pltpu.VMEM((klen + 1, width), F32),
        ),
        in_specs=[hbm] * 6,
        out_specs=(vmem, vmem, vmem, vmem),
        scratch_shapes=scratch,
        compiler_params=pltpu.CompilerParams(
            collective_id=0, has_side_effects=True, vmem_limit_bytes=65 * 1024 * 1000 - out_bytes
        ),
    )(glu_value, glu_gate, conv_taps, channel_gain[None, :], proj_weight, out_grad)
    if not fused:
        proj = lax.psum_scatter(proj, "sp", scatter_dimension=0, tiled=True)
        taps = lax.psum(taps, "sp")
    value_grad, gate_grad, proj, taps_grad, gain_grad = pl.pallas_call(
        finish_kernel,
        out_shape=(
            jax.ShapeDtypeStruct((rows, width), BF16),
            jax.ShapeDtypeStruct((rows, width), BF16),
            jax.ShapeDtypeStruct(proj.shape, F32),
            jax.ShapeDtypeStruct((klen, width), F32),
            jax.ShapeDtypeStruct((1, width), F32),
        ),
        in_specs=[vmem] * 4,
        out_specs=(hbm, hbm, hbm, vmem, vmem),
        scratch_shapes=[dma((3,))],
        compiler_params=pltpu.CompilerParams(vmem_limit_bytes=8 * 1024 * 1024),
    )(value_grad, gate_grad, proj, taps)
    return value_grad, gate_grad, proj, taps_grad, gain_grad[0]


def solution(mesh):
    from jax.sharding import PartitionSpec as P

    return jax.shard_map(
        per_device,
        mesh=mesh,
        in_specs=(
            P("sp", "tp"),
            P("sp", "tp"),
            P(None, "tp"),
            P("tp"),
            P("tp", None),
            P("sp", None),
        ),
        out_specs=(P("sp", "tp"), P("sp", "tp"), P(("tp", "sp"), None), P(None, "tp"), P("tp")),
        check_vma=False,
    )
```
